32 devices in a mesh: sp: 4 (over z), tp: 2 (over y), dp: 4 (over x, core).
Axes of the slice: x: 2, y: 2, z: 4, core: 2. Of those that a mesh axis runs over, the one named last changes fastest.
Arguments:
- latents: bfloat16 [4, 2048, 3072], P('dp', ('sp', 'tp')), may hold values from -5 to 5
- condition: bfloat16 [4, 3072], P('dp', ('sp', 'tp')), may hold values from -6 to 6
- context: bfloat16 [4, 384, 3072], P('dp', ('sp', 'tp')), may hold values from -6 to 6
- context_cond: bfloat16 [3072], P(('sp', 'tp')), may hold values from -6 to 6
- shift_weight: bfloat16 [3072, 3072], P(('sp', 'tp')), may hold values from -0.109375 to 0.109375
- scale_weight: bfloat16 [3072, 3072], P(('sp', 'tp')), may hold values from -0.109375 to 0.109375
- out_gate_weight: bfloat16 [3072, 3072], P(('sp', 'tp')), may hold values from -0.109375 to 0.109375
- pre_gain: float32 [3072], replicated, may hold values from 0.1 to 1.9
- post_gain: float32 [3072], replicated, may hold values from 0.1 to 1.9
- query_weight: bfloat16 [3072, 1024], P(None, 'tp'), may hold values from -0.108253175 to 0.108253175
- key_weight: bfloat16 [3072, 256], replicated, may hold values from -0.108253175 to 0.108253175
- value_weight: bfloat16 [3072, 256], replicated, may hold values from -0.109375 to 0.109375
- head_gate_weight: bfloat16 [3072, 1024], P(None, 'tp'), may hold values from -0.109375 to 0.109375
- lambdas: float32 [8], P('tp'), may hold values from 0.3 to 0.8
- head_gain: float32 [128], replicated, may hold values from 0.1 to 1.9
- out_weight: bfloat16 [1024, 3072], P(None, 'tp'), may hold values from -0.1875 to 0.1875
Outputs:
- mixed_out: bfloat16 [4, 2048, 3072], P('dp', ('sp', 'tp'))
The draws below stay inside these ranges and needn't reach their ends.
All inputs are finite; a program needn't handle non-finite values.
Results may differ from the reference program's by a relative error of at most 0.0128.
The reference program's roundings to bfloat16 on the way (of `silu_cond`, `silu_context`, `latent_in`, `context_in`, `weights`, `branch` and `projected`) count: a program that leaves them out, or rounds other values in their place, can miss the bound.
Values may be sent and summed in bfloat16 or wider, within the bound.
A program may use at most 64 MiB of HBM per device.

```python
import jax
import jax.numpy as jnp
from jax import lax

D = 3072
HEADS = 8
KVH = 2
HQK = 64
HV = 128
CTX = 384
SAMPLES = 4
LAT = 2048


def draw_latents(key, part):
    values = jnp.clip(jax.random.normal(jax.random.fold_in(key, 21), (SAMPLES, LAT, D), jnp.float32), -5.0, 5.0)
    return values.astype(jnp.bfloat16)


def draw_query_weight(key, part):
    values = jnp.clip(jax.random.normal(jax.random.fold_in(key, 31), (D, HEADS * 2 * HQK), jnp.float32), -5.0, 5.0) * D ** (-0.5)
    return values.astype(jnp.bfloat16)


def draw_key_weight(key, part):
    values = jnp.clip(jax.random.normal(jax.random.fold_in(key, 41), (D, KVH * 2 * HQK), jnp.float32), -5.0, 5.0) * D ** (-0.5)
    return values.astype(jnp.bfloat16)


def shard_levels(rng, shape, shards, least, high):
    factor_of, own = 1.0, jax.random.fold_in(rng, 6)
    for dim, shards_of in shards:
        heights = jnp.exp(jax.random.uniform(jax.random.fold_in(own, dim), (shards_of,), jnp.float32, least / len(shards), high / len(shards)))
        factor_of = factor_of * jnp.repeat(heights, shape[dim] // shards_of).reshape([-1 if axis == dim else 1 for axis in range(len(shape))])
    return factor_of


def noise(own_key, extent, scale, most, cuts=(), held_as=jnp.bfloat16):
    drawn = scale * jax.random.normal(own_key, extent, jnp.float32)
    if cuts:
        drawn = drawn * shard_levels(own_key, extent, cuts, -0.22, 0.18)
    return jnp.clip(drawn, -most, most).astype(held_as)


def setup_inputs(seed: int = 0) -> dict:
    key_of = jax.random.split(jax.random.key(seed), 17)
    return {
        "latents": draw_latents(jax.random.fold_in(key_of[16], 71), 0),
        "condition": noise(key_of[1], (SAMPLES, D), 1.0, 6.0, ((0, 4), (1, 8))),
        "context": noise(key_of[2], (SAMPLES, CTX, D), 1.0, 6.0, ((0, 4), (1, 8))),
        "context_cond": noise(key_of[3], (D,), 1.0, 6.0, ((0, 8),)),
        "shift_weight": noise(key_of[4], (D, D), D ** -0.5, 0.109375, ((0, 8),)),
        "scale_weight": noise(key_of[5], (D, D), D ** -0.5, 0.109375, ((0, 8),)),
        "out_gate_weight": noise(key_of[6], (D, D), D ** -0.5, 0.109375, ((0, 8),)),
        "pre_gain": jnp.clip(1.0 + 0.18 * jax.random.normal(key_of[7], (D,), jnp.float32), 0.1, 1.9),
        "post_gain": jnp.clip(1.0 + 0.18 * jax.random.normal(key_of[8], (D,), jnp.float32), 0.1, 1.9),
        "query_weight": draw_query_weight(jax.random.fold_in(key_of[16], 71), 0),
        "key_weight": draw_key_weight(jax.random.fold_in(key_of[16], 71), 0),
        "value_weight": noise(key_of[11], (D, KVH * HV), D ** -0.5, 0.109375),
        "head_gate_weight": noise(key_of[12], (D, HEADS * HV), D ** -0.5, 0.109375, ((1, 2),)),
        "lambdas": jnp.clip(0.3 + 0.5 * jax.random.uniform(key_of[13], (HEADS,), jnp.float32) ** shard_levels(key_of[13], (HEADS,), ((0, 2),), -0.2, 0.2), 0.3, 0.8),
        "head_gain": jnp.clip(1.0 + 0.18 * jax.random.normal(key_of[14], (HV,), jnp.float32), 0.1, 1.9),
        "out_weight": noise(key_of[15], (HEADS * HV, D), (HEADS * HV) ** -0.5, 0.1875, ((1, 2),)),
    }


NORM_EPSILON = 1e-06

def norm_rows(values, norm_gain):
    return values * lax.rsqrt(lax.optimization_barrier(jnp.mean(values * values, axis=-1, keepdims=True)) + NORM_EPSILON) * norm_gain

def rounded(values):
    return lax.optimization_barrier(values.astype(jnp.bfloat16))

def project(tokens, weight):
    flattened = tokens.reshape(-1, tokens.shape[-1])
    result = jnp.dot(flattened, weight, preferred_element_type=jnp.float32)
    return rounded(result).reshape(tokens.shape[:-1] + (weight.shape[1],))

def reference(latents, condition, context, context_cond, shift_weight, scale_weight, out_gate_weight, pre_gain, post_gain, query_weight, key_weight, value_weight, head_gate_weight, lambdas, head_gain, out_weight):
    silu_cond = rounded(jax.nn.silu(condition.astype(jnp.float32)))
    silu_context = rounded(jax.nn.silu(context_cond.astype(jnp.float32)))[None, :]
    shifts = jnp.dot(silu_cond, shift_weight, preferred_element_type=jnp.float32)
    scales = jnp.dot(silu_cond, scale_weight, preferred_element_type=jnp.float32)
    out_gate = jnp.dot(silu_cond, out_gate_weight, preferred_element_type=jnp.float32)
    context_shift = jnp.dot(silu_context, shift_weight, preferred_element_type=jnp.float32)
    context_scale = jnp.dot(silu_context, scale_weight, preferred_element_type=jnp.float32)
    latent_in = rounded(norm_rows(latents.astype(jnp.float32), pre_gain) * (1.0 + scales[:, None, :]) + shifts[:, None, :])
    context_in = rounded(norm_rows(context.astype(jnp.float32), pre_gain) * (1.0 + context_scale[:, None, :]) + context_shift[:, None, :])
    queries = project(latent_in, query_weight).reshape(SAMPLES, LAT, HEADS, 2, HQK)
    head_gate = project(latent_in, head_gate_weight).reshape(SAMPLES, LAT, HEADS, HV)
    joined = jnp.concatenate([context_in, latent_in], axis=1)
    key_rows = project(joined, key_weight).reshape(SAMPLES, CTX + LAT, KVH, 2, HQK)
    value_rows = project(joined, value_weight).reshape(SAMPLES, CTX + LAT, KVH, HV)
    group_size = HEADS // KVH

    def one_head(item_index):
        sample_index = item_index // HEADS
        head_index = item_index % HEADS
        key_group = head_index // group_size
        one_query = queries[sample_index, :, head_index].astype(jnp.float32)
        one_key = key_rows[sample_index, :, key_group].astype(jnp.float32)
        one_value = value_rows[sample_index, :, key_group].astype(jnp.float32)
        scores = jnp.einsum('qmd,kmd->mqk', one_query, one_key) * HQK ** (-0.5)
        largest = lax.optimization_barrier(jnp.max(scores, axis=-1, keepdims=True))
        exponent = jnp.exp(scores - largest)
        normalizer = lax.optimization_barrier(jnp.sum(exponent, axis=-1))
        weights = rounded(exponent).astype(jnp.float32)
        weighted = jnp.einsum('mqk,kv->mqv', weights, one_value)
        ratios = weighted / normalizer[..., None]
        attended = ratios[0] - lambdas[head_index] * ratios[1]
        gate_input = head_gate[sample_index, :, head_index].astype(jnp.float32)
        return rounded(norm_rows(attended, head_gain) * jax.nn.silu(gate_input))
    branch = lax.map(one_head, jnp.arange(SAMPLES * HEADS, dtype=jnp.int32))
    branch = branch.reshape(SAMPLES, HEADS, LAT, HV).transpose(0, 2, 1, 3).reshape(SAMPLES, LAT, HEADS * HV)
    projected = project(branch, out_weight)
    mixed_out = out_gate[:, None, :] * norm_rows(projected.astype(jnp.float32), post_gain)
    return mixed_out.astype(jnp.bfloat16)
```

```python
import functools
import math

import jax
import jax.numpy as jnp
from jax import lax
from jax.experimental import pallas as pl
from jax.experimental.pallas import tpu as pltpu
from jax.sharding import PartitionSpec as P

HEADS = 8
KVH = 2
HQK = 64
HV = 128
NORM_EPSILON = 1e-06
MESH = pl.DeviceIdType.MESH


def norm_rows(values, norm_gain):
    return (
        values
        * lax.rsqrt(jnp.mean(values * values, axis=-1, keepdims=True) + NORM_EPSILON)
        * norm_gain
    )


def modulate(tokens, norm_gain, shift, scale):
    values = norm_rows(tokens.astype(jnp.float32), norm_gain)
    return (values * (1.0 + scale) + shift).astype(jnp.bfloat16)


def project(tokens, weight):
    return jnp.dot(tokens, weight, preferred_element_type=jnp.float32).astype(jnp.bfloat16)


def shifted(values, axis, size, step):
    return lax.ppermute(values, axis, [(i, (i + step) % size) for i in range(size)])


def peer(offset, sp, tp):
    me = lax.axis_index("sp") * tp + lax.axis_index("tp")
    other = lax.rem(me + offset, sp * tp)
    return other // tp, lax.rem(other, tp)


def enter(sp, tp):
    barrier = pltpu.get_barrier_semaphore()
    for offset in range(1, sp * tp):
        row, column = peer(offset, sp, tp)
        pl.semaphore_signal(
            barrier, inc=1, device_id={"sp": row, "tp": column}, device_id_type=MESH
        )
    pl.semaphore_wait(barrier, sp * tp - 1)


def sum_kernel(sp, tp, part_ref, total_ref, held, send_sem, recv_sem):
    enter(sp, tp)
    copies = []
    for offset in range(1, sp * tp):
        row, column = peer(offset, sp, tp)
        copy = pltpu.make_async_remote_copy(
            src_ref=part_ref,
            dst_ref=held.at[offset - 1],
            send_sem=send_sem.at[offset - 1],
            recv_sem=recv_sem.at[offset - 1],
            device_id={"sp": row, "tp": column},
            device_id_type=MESH,
        )
        copy.start()
        copies.append(copy)
    total = part_ref[...]
    for offset, copy in enumerate(copies):
        copy.wait_recv()
        total = total + held[offset]
    total_ref[...] = total
    for copy in copies:
        copy.wait_send()


def sum_over_group(parts, sp, tp):
    others = sp * tp - 1
    return pl.pallas_call(
        functools.partial(sum_kernel, sp, tp),
        out_shape=jax.ShapeDtypeStruct(parts.shape, parts.dtype),
        in_specs=[pl.BlockSpec(memory_space=pltpu.VMEM)],
        out_specs=pl.BlockSpec(memory_space=pltpu.VMEM),
        scratch_shapes=[
            pltpu.VMEM((others,) + parts.shape, parts.dtype),
            pltpu.SemaphoreType.DMA((others,)),
            pltpu.SemaphoreType.DMA((others,)),
        ],
        compiler_params=pltpu.CompilerParams(collective_id=0, has_side_effects=True),
        cost_estimate=pl.CostEstimate(flops=10**6, bytes_accessed=20 * 10**6, transcendentals=0),
    )(parts)


def exchange_kernel(sp, tp, per_group, ckv_ref, lkv_ref, call_ref, lall_ref,
                    csend, crecv, lsend, lrecv, own_sem):
    own_group = lax.axis_index("tp") // per_group
    own_context = pltpu.make_async_copy(ckv_ref.at[own_group], call_ref.at[0], own_sem.at[0])
    own_latent = pltpu.make_async_copy(lkv_ref, lall_ref.at[0], own_sem.at[1])
    own_context.start()
    own_latent.start()
    enter(sp, tp)
    copies = []
    for step in range(1, sp):
        row = lax.rem(lax.axis_index("sp") + step, sp)
        copy = pltpu.make_async_remote_copy(
            src_ref=lkv_ref,
            dst_ref=lall_ref.at[step],
            send_sem=lsend.at[step - 1],
            recv_sem=lrecv.at[step - 1],
            device_id={"sp": row, "tp": lax.axis_index("tp")},
            device_id_type=MESH,
        )
        copy.start()
        copies.append(copy)
    for offset in range(1, sp * tp):
        row, column = peer(offset, sp, tp)
        copy = pltpu.make_async_remote_copy(
            src_ref=ckv_ref.at[column // per_group],
            dst_ref=call_ref.at[offset],
            send_sem=csend.at[offset - 1],
            recv_sem=crecv.at[offset - 1],
            device_id={"sp": row, "tp": column},
            device_id_type=MESH,
        )
        copy.start()
        copies.append(copy)
    own_context.wait()
    own_latent.wait()
    for copy in copies:
        copy.wait()


def exchange(context_kv, latent_kv, sp, tp, per_group):
    group = sp * tp
    return pl.pallas_call(
        functools.partial(exchange_kernel, sp, tp, per_group),
        out_shape=(
            jax.ShapeDtypeStruct((group,) + context_kv.shape[1:], context_kv.dtype),
            jax.ShapeDtypeStruct((sp,) + latent_kv.shape, latent_kv.dtype),
        ),
        in_specs=[pl.BlockSpec(memory_space=pltpu.VMEM)] * 2,
        out_specs=(pl.BlockSpec(memory_space=pltpu.VMEM),) * 2,
        scratch_shapes=[
            pltpu.SemaphoreType.DMA((group - 1,)),
            pltpu.SemaphoreType.DMA((group - 1,)),
            pltpu.SemaphoreType.DMA((max(sp - 1, 1),)),
            pltpu.SemaphoreType.DMA((max(sp - 1, 1),)),
            pltpu.SemaphoreType.DMA((2,)),
        ],
        compiler_params=pltpu.CompilerParams(collective_id=1, has_side_effects=True),
        cost_estimate=pl.CostEstimate(flops=10**6, bytes_accessed=30 * 10**6, transcendentals=0),
    )(context_kv, latent_kv)


def attend_kernel(lambda_ref, q_ref, gate_ref, gain_ref, ck_ref, cv_ref, lk_ref, lv_ref, out_ref):
    queries = q_ref[...]
    rows = queries.shape[0]
    lane = lax.broadcasted_iota(jnp.int32, queries.shape, 1)
    queries = (queries.astype(jnp.float32) * HQK ** (-0.5))
    both = jnp.concatenate(
        [jnp.where(lane < HQK, queries, 0.0), jnp.where(lane < HQK, 0.0, queries)], axis=0
    ).astype(jnp.bfloat16)
    contract = (((1,), (1,)), ((), ()))
    first = lax.dot_general(both, ck_ref[...], contract, preferred_element_type=jnp.float32)
    second = lax.dot_general(both, lk_ref[...], contract, preferred_element_type=jnp.float32)
    largest = jnp.maximum(
        jnp.max(first, axis=-1, keepdims=True), jnp.max(second, axis=-1, keepdims=True)
    )
    first = jnp.exp(first - largest)
    second = jnp.exp(second - largest)
    normalizer = jnp.sum(first, axis=-1, keepdims=True) + jnp.sum(second, axis=-1, keepdims=True)
    weighted = jnp.dot(
        first.astype(jnp.bfloat16), cv_ref[...], preferred_element_type=jnp.float32
    ) + jnp.dot(second.astype(jnp.bfloat16), lv_ref[...], preferred_element_type=jnp.float32)
    ratios = weighted / normalizer
    attended = ratios[:rows] - lambda_ref[pl.program_id(0)] * ratios[rows:]
    gate = jax.nn.silu(gate_ref[...].astype(jnp.float32))
    out_ref[...] = (norm_rows(attended, gain_ref[...]) * gate).astype(jnp.bfloat16)


def attend(lambdas, queries, gate, head_gain, context_kv, latent_kv):
    rows, width = queries.shape
    heads = width // (2 * HQK)
    block = math.gcd(rows, 128)
    keys = context_kv.shape[0] + latent_kv.shape[0]

    def whole(part, column):
        return pl.BlockSpec((part.shape[0], 128), lambda h, i: (0, column))

    tile = pl.BlockSpec((block, 128), lambda h, i: (i, h))
    return pl.pallas_call(
        attend_kernel,
        grid=(heads, rows // block),
        out_shape=jax.ShapeDtypeStruct((rows, heads * HV), jnp.bfloat16),
        in_specs=[
            pl.BlockSpec(memory_space=pltpu.SMEM),
            tile,
            tile,
            pl.BlockSpec((1, HV), lambda h, i: (0, 0)),
            whole(context_kv, 0),
            whole(context_kv, 1),
            whole(latent_kv, 0),
            whole(latent_kv, 1),
        ],
        out_specs=tile,
        compiler_params=pltpu.CompilerParams(vmem_limit_bytes=48 * 2**20),
        cost_estimate=pl.CostEstimate(
            flops=16 * heads * rows * keys * HV, bytes_accessed=4 * 10**6,
            transcendentals=2 * heads * rows * keys,
        ),
    )(lambdas, queries, gate, head_gain, context_kv, context_kv, latent_kv, latent_kv)


def tail_kernel(tp, dp, *refs):
    branches, refs = refs[:tp], refs[tp:]
    own_weight, refs = refs[0], refs[1:]
    pieces, refs = refs[: (tp - 1) * dp], refs[(tp - 1) * dp :]
    out_gate_ref, gain_ref, out_ref, branch, projected = refs
    me, mine = lax.axis_index("tp"), lax.axis_index("dp")
    width = branches[0].shape[1]
    columns = own_weight.shape[1]
    depth = own_weight.shape[0] // dp
    for step in range(tp):
        owner = lax.rem(me + step, tp)
        branch[:, pl.ds(pl.multiple_of(owner * width, width), width)] = branches[step][...]
    projected[:, pl.ds(pl.multiple_of(me * columns, columns), columns)] = jnp.dot(
        branch[...], own_weight[...], preferred_element_type=jnp.float32
    )
    for step in range(1, tp):
        owner = lax.rem(me - step + tp, tp)
        total = None
        for turn in range(dp):
            source = lax.rem(mine - turn + dp, dp)
            part = jnp.dot(
                branch[:, pl.ds(pl.multiple_of(source * depth, depth), depth)],
                pieces[(step - 1) * dp + turn][...],
                preferred_element_type=jnp.float32,
            )
            total = part if total is None else total + part
        projected[:, pl.ds(pl.multiple_of(owner * columns, columns), columns)] = total
    values = projected[...].astype(jnp.bfloat16).astype(jnp.float32)
    out_ref[...] = (out_gate_ref[...] * norm_rows(values, gain_ref[...])).astype(jnp.bfloat16)


def tail(branches, own_weight, pieces, out_gate, post_gain, tp, dp):
    rows = branches[0].shape[0]
    width = post_gain.shape[1]
    operands = (*branches, own_weight, *pieces, out_gate, post_gain)
    return pl.pallas_call(
        functools.partial(tail_kernel, tp, dp),
        out_shape=jax.ShapeDtypeStruct((rows, width), jnp.bfloat16),
        in_specs=[pl.BlockSpec(memory_space=pltpu.VMEM)] * len(operands),
        out_specs=pl.BlockSpec(memory_space=pltpu.VMEM),
        scratch_shapes=[
            pltpu.VMEM((rows, own_weight.shape[0]), jnp.bfloat16),
            pltpu.VMEM((rows, width), jnp.float32),
        ],
        compiler_params=pltpu.CompilerParams(vmem_limit_bytes=48 * 2**20),
        cost_estimate=pl.CostEstimate(
            flops=2 * rows * width * own_weight.shape[0], bytes_accessed=10**7, transcendentals=0
        ),
    )(*operands)


def local(
    sp,
    tp,
    dp,
    latents,
    condition,
    context,
    context_cond,
    shift_weight,
    scale_weight,
    out_gate_weight,
    pre_gain,
    post_gain,
    query_weight,
    key_weight,
    value_weight,
    head_gate_weight,
    lambdas,
    head_gain,
    out_weight,
):
    pair_width = 2 * HQK
    local_heads = query_weight.shape[1] // pair_width
    per_group = (HEADS // KVH) // local_heads
    key_group = lax.axis_index("tp") // per_group
    own = latents[0]
    rows = own.shape[0]
    blocks = [own] + [shifted(own, "tp", tp, step) for step in range(1, tp)]

    conditions = jnp.concatenate([condition, context_cond[None, :]], axis=0).astype(jnp.float32)
    conditions = jax.nn.silu(conditions).astype(jnp.bfloat16)
    parts = jnp.concatenate(
        [
            jnp.dot(conditions, shift_weight, preferred_element_type=jnp.float32),
            jnp.dot(conditions, scale_weight, preferred_element_type=jnp.float32),
            jnp.dot(conditions[:1], out_gate_weight, preferred_element_type=jnp.float32),
        ],
        axis=0,
    )
    sums = sum_over_group(parts, sp, tp)
    shift, context_shift, scale, context_scale, out_gate = (
        sums[0:1], sums[1:2], sums[2:3], sums[3:4], sums[4:5]
    )

    depth = out_weight.shape[0] // dp
    share = lax.dynamic_slice_in_dim(out_weight, lax.axis_index("dp") * depth, depth, 0)
    held = lax.optimization_barrier((share, *blocks[1:]))
    share, blocks = held[0], [own, *held[1:]]
    pieces = []
    for step in range(1, tp):
        arrived = shifted(share, "tp", tp, step)
        pieces.append(arrived)
        pieces.extend(shifted(arrived, "dp", dp, turn) for turn in range(1, dp))

    context_in = modulate(context[0], pre_gain, context_shift, context_scale)
    context_keys = project(context_in, key_weight)
    context_values = project(context_in, value_weight)
    context_kv = jnp.stack(
        [
            jnp.concatenate(
                [
                    context_keys[:, g * pair_width : (g + 1) * pair_width],
                    context_values[:, g * HV : (g + 1) * HV],
                ],
                axis=1,
            )
            for g in range(KVH)
        ]
    )

    own_key_weight = lax.dynamic_slice_in_dim(key_weight, key_group * pair_width, pair_width, 1)
    own_value_weight = lax.dynamic_slice_in_dim(value_weight, key_group * HV, HV, 1)
    kv_weight = jnp.concatenate([own_key_weight, own_value_weight], axis=1)
    latent_in = modulate(jnp.concatenate(blocks, axis=0), pre_gain, shift, scale)
    latent_kv = project(latent_in, kv_weight)
    queries = project(latent_in, query_weight)
    head_gate = project(latent_in, head_gate_weight)

    context_all, latent_all = exchange(context_kv, latent_kv, sp, tp, per_group)
    context_all = context_all.reshape(-1, context_all.shape[-1])
    latent_all = latent_all.reshape(-1, latent_all.shape[-1])
    branch = attend(lambdas, queries, head_gate, head_gain[None, :], context_all, latent_all)

    branches = [branch[:rows]]
    for step in range(1, tp):
        block = branch[step * rows : (step + 1) * rows]
        branches.append(shifted(block, "tp", tp, tp - step))
    result = tail(branches, out_weight, pieces, out_gate, post_gain[None, :], tp, dp)
    return result[None]


def solution(mesh):
    return jax.shard_map(
        functools.partial(local, mesh.shape["sp"], mesh.shape["tp"], mesh.shape["dp"]),
        mesh=mesh,
        in_specs=(
            P("dp", ("sp", "tp"), None),
            P("dp", ("sp", "tp")),
            P("dp", ("sp", "tp"), None),
            P(("sp", "tp")),
            P(("sp", "tp"), None),
            P(("sp", "tp"), None),
            P(("sp", "tp"), None),
            P(),
            P(),
            P(None, "tp"),
            P(),
            P(),
            P(None, "tp"),
            P("tp"),
            P(),
            P(None, "tp"),
        ),
        out_specs=P("dp", ("sp", "tp"), None),
        check_vma=False,
    )
```

```python
import functools
import math

import jax
import jax.numpy as jnp
from jax import lax
from jax.experimental import pallas as pl
from jax.experimental.pallas import tpu as pltpu
from jax.sharding import PartitionSpec as P


HEADS = 8
KVH = 2
HQK = 64
HV = 128
NORM_EPSILON = 1e-06
MESH = pl.DeviceIdType.MESH


def norm_rows(values, norm_gain):
    return (
        values
        * lax.rsqrt(jnp.mean(values * values, axis=-1, keepdims=True) + NORM_EPSILON)
        * norm_gain
    )


def modulate(tokens, norm_gain, shift, scale):
    values = norm_rows(tokens.astype(jnp.float32), norm_gain)
    return (values * (1.0 + scale) + shift).astype(jnp.bfloat16)


def project(tokens, weight):
    return jnp.dot(tokens, weight, preferred_element_type=jnp.float32).astype(jnp.bfloat16)


def shifted(values, axis, size, step):
    return lax.ppermute(values, axis, [(i, (i + step) % size) for i in range(size)])


def peer(offset, sp, tp):
    me = lax.axis_index("sp") * tp + lax.axis_index("tp")
    other = lax.rem(me + offset, sp * tp)
    return other // tp, lax.rem(other, tp)


def enter(sp, tp):
    barrier = pltpu.get_barrier_semaphore()
    for offset in range(1, sp * tp):
        row, column = peer(offset, sp, tp)
        pl.semaphore_signal(
            barrier, inc=1, device_id={"sp": row, "tp": column}, device_id_type=MESH
        )
    pl.semaphore_wait(barrier, sp * tp - 1)


def sum_kernel(sp, tp, part_ref, total_ref, held, send_sem, recv_sem):
    enter(sp, tp)
    copies = []
    for offset in range(1, sp * tp):
        row, column = peer(offset, sp, tp)
        copy = pltpu.make_async_remote_copy(
            src_ref=part_ref,
            dst_ref=held.at[offset - 1],
            send_sem=send_sem.at[offset - 1],
            recv_sem=recv_sem.at[offset - 1],
            device_id={"sp": row, "tp": column},
            device_id_type=MESH,
        )
        copy.start()
        copies.append(copy)
    total = part_ref[...]
    for offset, copy in enumerate(copies):
        copy.wait_recv()
        total = total + held[offset]
    total_ref[...] = total
    for copy in copies:
        copy.wait_send()


def sum_over_group(parts, sp, tp):
    others = sp * tp - 1
    return pl.pallas_call(
        functools.partial(sum_kernel, sp, tp),
        out_shape=jax.ShapeDtypeStruct(parts.shape, parts.dtype),
        in_specs=[pl.BlockSpec(memory_space=pltpu.VMEM)],
        out_specs=pl.BlockSpec(memory_space=pltpu.VMEM),
        scratch_shapes=[
            pltpu.VMEM((others,) + parts.shape, parts.dtype),
            pltpu.SemaphoreType.DMA((others,)),
            pltpu.SemaphoreType.DMA((others,)),
        ],
        compiler_params=pltpu.CompilerParams(collective_id=0, has_side_effects=True),
        cost_estimate=pl.CostEstimate(flops=10**6, bytes_accessed=20 * 10**6, transcendentals=0),
    )(parts)


def attend_kernel(count, lambda_ref, q_ref, gate_ref, gain_ref, *refs):
    key_refs, value_refs, out_ref = refs[:count], refs[count : 2 * count], refs[2 * count]
    queries = q_ref[...]
    rows = queries.shape[0]
    lane = lax.broadcasted_iota(jnp.int32, queries.shape, 1)
    queries = (queries.astype(jnp.float32) * HQK ** (-0.5))
    both = jnp.concatenate(
        [jnp.where(lane < HQK, queries, 0.0), jnp.where(lane < HQK, 0.0, queries)], axis=0
    ).astype(jnp.bfloat16)
    contract = (((1,), (1,)), ((), ()))
    keys = jnp.concatenate([ref[...] for ref in key_refs], axis=0)
    values = jnp.concatenate([ref[...] for ref in value_refs], axis=0)
    scores = lax.dot_general(both, keys, contract, preferred_element_type=jnp.float32)
    largest = jnp.max(scores, axis=-1, keepdims=True)
    exponent = jnp.exp(scores - largest)
    normalizer = jnp.sum(exponent, axis=-1, keepdims=True)
    weighted = jnp.dot(exponent.astype(jnp.bfloat16), values, preferred_element_type=jnp.float32)
    ratios = weighted / normalizer
    attended = ratios[:rows] - lambda_ref[pl.program_id(0)] * ratios[rows:]
    gate = jax.nn.silu(gate_ref[...].astype(jnp.float32))
    out_ref[...] = (norm_rows(attended, gain_ref[...]) * gate).astype(jnp.bfloat16)


def attend(lambdas, queries, gate, head_gain, parts):
    rows, width = queries.shape
    heads = width // (2 * HQK)
    block = math.gcd(rows, 128)
    keys = sum(part.shape[0] for part in parts)

    def whole(part, column):
        return pl.BlockSpec((part.shape[0], 128), lambda h, i: (0, column))

    tile = pl.BlockSpec((block, 128), lambda h, i: (i, h))
    return pl.pallas_call(
        functools.partial(attend_kernel, len(parts)),
        grid=(heads, rows // block),
        out_shape=jax.ShapeDtypeStruct((rows, heads * HV), jnp.bfloat16),
        in_specs=[
            pl.BlockSpec(memory_space=pltpu.SMEM),
            tile,
            tile,
            pl.BlockSpec((1, HV), lambda h, i: (0, 0)),
            *(whole(part, 0) for part in parts),
            *(whole(part, 1) for part in parts),
        ],
        out_specs=tile,
        compiler_params=pltpu.CompilerParams(vmem_limit_bytes=48 * 2**20),
        cost_estimate=pl.CostEstimate(
            flops=16 * heads * rows * keys * HV, bytes_accessed=4 * 10**6,
            transcendentals=2 * heads * rows * keys,
        ),
    )(lambdas, queries, gate, head_gain, *parts, *parts)


def tail_kernel(tp, dp, *refs):
    branches, refs = refs[:tp], refs[tp:]
    own_weight, refs = refs[0], refs[1:]
    pieces, refs = refs[: (tp - 1) * dp], refs[(tp - 1) * dp :]
    out_gate_ref, gain_ref, out_ref, branch, projected = refs
    me, mine = lax.axis_index("tp"), lax.axis_index("dp")
    width = branches[0].shape[1]
    columns = own_weight.shape[1]
    depth = own_weight.shape[0] // dp
    for step in range(tp):
        owner = lax.rem(me + step, tp)
        branch[:, pl.ds(pl.multiple_of(owner * width, width), width)] = branches[step][...]
    projected[:, pl.ds(pl.multiple_of(me * columns, columns), columns)] = jnp.dot(
        branch[...], own_weight[...], preferred_element_type=jnp.float32
    )
    for step in range(1, tp):
        owner = lax.rem(me - step + tp, tp)
        total = None
        for turn in range(dp):
            source = lax.bitwise_xor(mine, turn)
            part = jnp.dot(
                branch[:, pl.ds(pl.multiple_of(source * depth, depth), depth)],
                pieces[(step - 1) * dp + turn][...],
                preferred_element_type=jnp.float32,
            )
            total = part if total is None else total + part
        projected[:, pl.ds(pl.multiple_of(owner * columns, columns), columns)] = total
    values = projected[...].astype(jnp.bfloat16).astype(jnp.float32)
    out_ref[...] = (out_gate_ref[...] * norm_rows(values, gain_ref[...])).astype(jnp.bfloat16)


def tail(branches, own_weight, pieces, out_gate, post_gain, tp, dp):
    rows = branches[0].shape[0]
    width = post_gain.shape[1]
    operands = (*branches, own_weight, *pieces, out_gate, post_gain)
    return pl.pallas_call(
        functools.partial(tail_kernel, tp, dp),
        out_shape=jax.ShapeDtypeStruct((rows, width), jnp.bfloat16),
        in_specs=[pl.BlockSpec(memory_space=pltpu.VMEM)] * len(operands),
        out_specs=pl.BlockSpec(memory_space=pltpu.VMEM),
        scratch_shapes=[
            pltpu.VMEM((rows, own_weight.shape[0]), jnp.bfloat16),
            pltpu.VMEM((rows, width), jnp.float32),
        ],
        compiler_params=pltpu.CompilerParams(vmem_limit_bytes=48 * 2**20),
        cost_estimate=pl.CostEstimate(
            flops=2 * rows * width * own_weight.shape[0], bytes_accessed=10**7, transcendentals=0
        ),
    )(*operands)


def local(
    sp,
    tp,
    dp,
    latents,
    condition,
    context,
    context_cond,
    shift_weight,
    scale_weight,
    out_gate_weight,
    pre_gain,
    post_gain,
    query_weight,
    key_weight,
    value_weight,
    head_gate_weight,
    lambdas,
    head_gain,
    out_weight,
):
    pair_width = 2 * HQK
    local_heads = query_weight.shape[1] // pair_width
    per_group = (HEADS // KVH) // local_heads
    key_group = lax.axis_index("tp") // per_group
    own = latents[0]
    rows = own.shape[0]
    early = rows // 4
    steps = range(1, tp)
    heads_up = [shifted(own[:early], "tp", tp, step) for step in steps]

    conditions = jnp.concatenate([condition, context_cond[None, :]], axis=0).astype(jnp.float32)
    conditions = jax.nn.silu(conditions).astype(jnp.bfloat16)
    parts = jnp.concatenate(
        [
            jnp.dot(conditions, shift_weight, preferred_element_type=jnp.float32),
            jnp.dot(conditions, scale_weight, preferred_element_type=jnp.float32),
            jnp.dot(conditions[:1], out_gate_weight, preferred_element_type=jnp.float32),
        ],
        axis=0,
    )
    sums = sum_over_group(parts, sp, tp)
    late, sums = lax.optimization_barrier((own[early:], sums))
    shift, context_shift, scale, context_scale, out_gate = (
        sums[0:1], sums[1:2], sums[2:3], sums[3:4], sums[4:5]
    )
    rest = [shifted(late, "tp", tp, step) for step in steps]

    own_key_weight = lax.dynamic_slice_in_dim(key_weight, key_group * pair_width, pair_width, 1)
    own_value_weight = lax.dynamic_slice_in_dim(value_weight, key_group * HV, HV, 1)
    kv_weight = jnp.concatenate([own_key_weight, own_value_weight], axis=1)

    def spread(values):
        return [values] + [shifted(values, "sp", sp, step) for step in range(1, sp)]

    own_in = modulate(own, pre_gain, shift, scale)
    own_kv = project(own_in, kv_weight)
    own_kv = spread(own_kv)
    own_queries = project(own_in, query_weight)
    own_gate = project(own_in, head_gate_weight)

    context_in = modulate(context[0], pre_gain, context_shift, context_scale)
    context_kv = jnp.concatenate(
        [project(context_in, key_weight), project(context_in, value_weight)], axis=1
    )
    contexts = [context_kv] + [shifted(context_kv, "tp", tp, step) for step in steps]
    contexts = [
        jnp.concatenate(
            [
                lax.dynamic_slice_in_dim(part, key_group * pair_width, pair_width, 1),
                lax.dynamic_slice_in_dim(part, KVH * pair_width + key_group * HV, HV, 1),
            ],
            axis=1,
        )
        for part in contexts
    ]

    depth = out_weight.shape[0] // dp
    share = lax.dynamic_slice_in_dim(out_weight, lax.axis_index("dp") * depth, depth, 0)
    share, *rest = lax.optimization_barrier((share, *rest))
    pieces = []
    for step in steps:
        turns = {0: shifted(share, "tp", tp, step)}
        bit = dp // 2
        while bit:
            for turn in list(turns):
                turns[turn ^ bit] = lax.ppermute(
                    turns[turn], "dp", [(i, i ^ bit) for i in range(dp)]
                )
            bit //= 2
        pieces.extend(turns[turn] for turn in range(dp))

    other_in = modulate(
        jnp.concatenate([part for pair in zip(heads_up, rest) for part in pair], axis=0),
        pre_gain, shift, scale,
    )
    other_kv = spread(jnp.concatenate([project(other_in, kv_weight), *contexts], axis=0))
    other_queries = project(other_in, query_weight)
    other_gate = project(other_in, head_gate_weight)

    keys = own_kv + other_kv
    gain = head_gain[None, :]
    other_branch = attend(lambdas, other_queries, other_gate, gain, keys)
    returned = [
        shifted(other_branch[(step - 1) * rows : step * rows], "tp", tp, tp - step)
        for step in steps
    ]
    own_branch = attend(lambdas, own_queries, own_gate, gain, keys)
    branches = [own_branch, *returned]
    result = tail(branches, out_weight, pieces, out_gate, post_gain[None, :], tp, dp)
    return result[None]


def solution(mesh):
    return jax.shard_map(
        functools.partial(local, mesh.shape["sp"], mesh.shape["tp"], mesh.shape["dp"]),
        mesh=mesh,
        in_specs=(
            P("dp", ("sp", "tp"), None),
            P("dp", ("sp", "tp")),
            P("dp", ("sp", "tp"), None),
            P(("sp", "tp")),
            P(("sp", "tp"), None),
            P(("sp", "tp"), None),
            P(("sp", "tp"), None),
            P(),
            P(),
            P(None, "tp"),
            P(),
            P(),
            P(None, "tp"),
            P("tp"),
            P(),
            P(None, "tp"),
        ),
        out_specs=P("dp", ("sp", "tp"), None),
        check_vma=False,
    )
```

```python
import functools
import math

import jax
import jax.numpy as jnp
from jax import lax
from jax.experimental import pallas as pl
from jax.experimental.pallas import tpu as pltpu
from jax.sharding import PartitionSpec as P


HEADS = 8
KVH = 2
HQK = 64
HV = 128
NORM_EPSILON = 1e-06
MESH = pl.DeviceIdType.MESH


def norm_rows(values, norm_gain):
    return (
        values
        * lax.rsqrt(jnp.mean(values * values, axis=-1, keepdims=True) + NORM_EPSILON)
        * norm_gain
    )


def modulate(tokens, norm_gain, shift, scale):
    values = norm_rows(tokens.astype(jnp.float32), norm_gain)
    return (values * (1.0 + scale) + shift).astype(jnp.bfloat16)


def project(tokens, weight):
    return jnp.dot(tokens, weight, preferred_element_type=jnp.float32).astype(jnp.bfloat16)


def shifted(values, axis, size, step):
    return lax.ppermute(values, axis, [(i, (i + step) % size) for i in range(size)])


def peer(offset, sp, tp):
    me = lax.axis_index("sp") * tp + lax.axis_index("tp")
    other = lax.rem(me + offset, sp * tp)
    return other // tp, lax.rem(other, tp)


def enter(sp, tp):
    barrier = pltpu.get_barrier_semaphore()
    for offset in range(1, sp * tp):
        row, column = peer(offset, sp, tp)
        pl.semaphore_signal(
            barrier, inc=1, device_id={"sp": row, "tp": column}, device_id_type=MESH
        )
    pl.semaphore_wait(barrier, sp * tp - 1)


def sum_kernel(sp, tp, part_ref, total_ref, held, send_sem, recv_sem):
    enter(sp, tp)
    copies = []
    for offset in range(1, sp * tp):
        row, column = peer(offset, sp, tp)
        copy = pltpu.make_async_remote_copy(
            src_ref=part_ref,
            dst_ref=held.at[offset - 1],
            send_sem=send_sem.at[offset - 1],
            recv_sem=recv_sem.at[offset - 1],
            device_id={"sp": row, "tp": column},
            device_id_type=MESH,
        )
        copy.start()
        copies.append(copy)
    total = part_ref[...]
    for offset, copy in enumerate(copies):
        copy.wait_recv()
        total = total + held[offset]
    total_ref[...] = total
    for copy in copies:
        copy.wait_send()


def sum_over_group(parts, sp, tp):
    others = sp * tp - 1
    return pl.pallas_call(
        functools.partial(sum_kernel, sp, tp),
        out_shape=jax.ShapeDtypeStruct(parts.shape, parts.dtype),
        in_specs=[pl.BlockSpec(memory_space=pltpu.VMEM)],
        out_specs=pl.BlockSpec(memory_space=pltpu.VMEM),
        scratch_shapes=[
            pltpu.VMEM((others,) + parts.shape, parts.dtype),
            pltpu.SemaphoreType.DMA((others,)),
            pltpu.SemaphoreType.DMA((others,)),
        ],
        compiler_params=pltpu.CompilerParams(collective_id=0, has_side_effects=True),
        cost_estimate=pl.CostEstimate(flops=10**6, bytes_accessed=20 * 10**6, transcendentals=0),
    )(parts)


def attend_kernel(count, lambda_ref, q_ref, gate_ref, gain_ref, *refs):
    key_refs, value_refs, out_ref = refs[:count], refs[count : 2 * count], refs[2 * count]
    queries = q_ref[...]
    rows = queries.shape[0]
    lane = lax.broadcasted_iota(jnp.int32, queries.shape, 1)
    queries = (queries.astype(jnp.float32) * HQK ** (-0.5))
    both = jnp.concatenate(
        [jnp.where(lane < HQK, queries, 0.0), jnp.where(lane < HQK, 0.0, queries)], axis=0
    ).astype(jnp.bfloat16)
    contract = (((1,), (1,)), ((), ()))
    keys = jnp.concatenate([ref[...] for ref in key_refs], axis=0)
    values = jnp.concatenate([ref[...] for ref in value_refs], axis=0)
    scores = lax.dot_general(both, keys, contract, preferred_element_type=jnp.float32)
    largest = jnp.max(scores, axis=-1, keepdims=True)
    exponent = jnp.exp(scores - largest)
    normalizer = jnp.sum(exponent, axis=-1, keepdims=True)
    weighted = jnp.dot(exponent.astype(jnp.bfloat16), values, preferred_element_type=jnp.float32)
    ratios = weighted / normalizer
    attended = ratios[:rows] - lambda_ref[pl.program_id(0)] * ratios[rows:]
    gate = jax.nn.silu(gate_ref[...].astype(jnp.float32))
    out_ref[...] = (norm_rows(attended, gain_ref[...]) * gate).astype(jnp.bfloat16)


def attend(lambdas, queries, gate, head_gain, parts):
    rows, width = queries.shape
    heads = width // (2 * HQK)
    block = math.gcd(rows, 128)
    keys = sum(part.shape[0] for part in parts)

    def whole(part, column):
        return pl.BlockSpec((part.shape[0], 128), lambda h, i: (0, column))

    tile = pl.BlockSpec((block, 128), lambda h, i: (i, h))
    return pl.pallas_call(
        functools.partial(attend_kernel, len(parts)),
        grid=(heads, rows // block),
        out_shape=jax.ShapeDtypeStruct((rows, heads * HV), jnp.bfloat16),
        in_specs=[
            pl.BlockSpec(memory_space=pltpu.SMEM),
            tile,
            tile,
            pl.BlockSpec((1, HV), lambda h, i: (0, 0)),
            *(whole(part, 0) for part in parts),
            *(whole(part, 1) for part in parts),
        ],
        out_specs=tile,
        compiler_params=pltpu.CompilerParams(vmem_limit_bytes=48 * 2**20),
        cost_estimate=pl.CostEstimate(
            flops=16 * heads * rows * keys * HV, bytes_accessed=4 * 10**6,
            transcendentals=2 * heads * rows * keys,
        ),
    )(lambdas, queries, gate, head_gain, *parts, *parts)


def tail_kernel(tp, dp, *refs):
    branches, refs = refs[:tp], refs[tp:]
    own_weight, refs = refs[0], refs[1:]
    pieces, refs = refs[: (tp - 1) * dp], refs[(tp - 1) * dp :]
    out_gate_ref, gain_ref, out_ref, branch, projected = refs
    me, mine = lax.axis_index("tp"), lax.axis_index("dp")
    width = branches[0].shape[1]
    columns = own_weight.shape[1]
    depth = own_weight.shape[0] // dp
    for step in range(tp):
        owner = lax.rem(me + step, tp)
        branch[:, pl.ds(pl.multiple_of(owner * width, width), width)] = branches[step][...]
    projected[:, pl.ds(pl.multiple_of(me * columns, columns), columns)] = jnp.dot(
        branch[...], own_weight[...], preferred_element_type=jnp.float32
    )
    for step in range(1, tp):
        owner = lax.rem(me - step + tp, tp)
        total = None
        for turn in range(dp):
            source = lax.bitwise_xor(mine, turn)
            part = jnp.dot(
                branch[:, pl.ds(pl.multiple_of(source * depth, depth), depth)],
                pieces[(step - 1) * dp + turn][...],
                preferred_element_type=jnp.float32,
            )
            total = part if total is None else total + part
        projected[:, pl.ds(pl.multiple_of(owner * columns, columns), columns)] = total
    values = projected[...].astype(jnp.bfloat16).astype(jnp.float32)
    out_ref[...] = (out_gate_ref[...] * norm_rows(values, gain_ref[...])).astype(jnp.bfloat16)


def tail(branches, own_weight, pieces, out_gate, post_gain, tp, dp):
    rows = branches[0].shape[0]
    width = post_gain.shape[1]
    operands = (*branches, own_weight, *pieces, out_gate, post_gain)
    return pl.pallas_call(
        functools.partial(tail_kernel, tp, dp),
        out_shape=jax.ShapeDtypeStruct((rows, width), jnp.bfloat16),
        in_specs=[pl.BlockSpec(memory_space=pltpu.VMEM)] * len(operands),
        out_specs=pl.BlockSpec(memory_space=pltpu.VMEM),
        scratch_shapes=[
            pltpu.VMEM((rows, own_weight.shape[0]), jnp.bfloat16),
            pltpu.VMEM((rows, width), jnp.float32),
        ],
        compiler_params=pltpu.CompilerParams(vmem_limit_bytes=48 * 2**20),
        cost_estimate=pl.CostEstimate(
            flops=2 * rows * width * own_weight.shape[0], bytes_accessed=10**7, transcendentals=0
        ),
    )(*operands)


def local(
    sp,
    tp,
    dp,
    latents,
    condition,
    context,
    context_cond,
    shift_weight,
    scale_weight,
    out_gate_weight,
    pre_gain,
    post_gain,
    query_weight,
    key_weight,
    value_weight,
    head_gate_weight,
    lambdas,
    head_gain,
    out_weight,
):
    pair_width = 2 * HQK
    local_heads = query_weight.shape[1] // pair_width
    per_group = (HEADS // KVH) // local_heads
    key_group = lax.axis_index("tp") // per_group
    own = latents[0]
    rows = own.shape[0]
    early = rows // 4
    steps = range(1, tp)
    heads_up = [shifted(own[:early], "tp", tp, step) for step in steps]

    conditions = jnp.concatenate([condition, context_cond[None, :]], axis=0).astype(jnp.float32)
    conditions = jax.nn.silu(conditions).astype(jnp.bfloat16)
    parts = jnp.concatenate(
        [
            jnp.dot(conditions, shift_weight, preferred_element_type=jnp.float32),
            jnp.dot(conditions, scale_weight, preferred_element_type=jnp.float32),
            jnp.dot(conditions[:1], out_gate_weight, preferred_element_type=jnp.float32),
        ],
        axis=0,
    )
    sums = sum_over_group(parts, sp, tp)
    late, sums = lax.optimization_barrier((own[early:], sums))
    shift, context_shift, scale, context_scale, out_gate = (
        sums[0:1], sums[1:2], sums[2:3], sums[3:4], sums[4:5]
    )
    rest = [shifted(late, "tp", tp, step) for step in steps]

    own_key_weight = lax.dynamic_slice_in_dim(key_weight, key_group * pair_width, pair_width, 1)
    own_value_weight = lax.dynamic_slice_in_dim(value_weight, key_group * HV, HV, 1)
    kv_weight = jnp.concatenate([own_key_weight, own_value_weight], axis=1)

    def spread(values):
        return [values] + [shifted(values, "sp", sp, step) for step in range(1, sp)]

    own_in = modulate(own, pre_gain, shift, scale)
    own_kv = project(own_in, kv_weight)
    own_kv = spread(own_kv)
    own_queries = project(own_in, query_weight)
    own_gate = project(own_in, head_gate_weight)

    context_in = modulate(context[0], pre_gain, context_shift, context_scale)
    context_kv = jnp.concatenate(
        [project(context_in, key_weight), project(context_in, value_weight)], axis=1
    )
    contexts = [context_kv] + [shifted(context_kv, "tp", tp, step) for step in steps]
    contexts = [
        jnp.concatenate(
            [
                lax.dynamic_slice_in_dim(part, key_group * pair_width, pair_width, 1),
                lax.dynamic_slice_in_dim(part, KVH * pair_width + key_group * HV, HV, 1),
            ],
            axis=1,
        )
        for part in contexts
    ]

    depth = out_weight.shape[0] // dp
    share = lax.dynamic_slice_in_dim(out_weight, lax.axis_index("dp") * depth, depth, 0)
    share, *rest = lax.optimization_barrier((share, *rest))
    firsts = [shifted(share, "tp", tp, step) for step in steps]

    other_in = modulate(
        jnp.concatenate([part for pair in zip(heads_up, rest) for part in pair], axis=0),
        pre_gain, shift, scale,
    )
    other_kv = jnp.concatenate([project(other_in, kv_weight), *contexts], axis=0)
    other_kv = spread(other_kv)
    other_queries = project(other_in, query_weight)
    other_gate = project(other_in, head_gate_weight)

    held = lax.optimization_barrier((*firsts, *other_kv))
    firsts, other_kv = held[: tp - 1], list(held[tp - 1 :])
    pieces = []
    for first in firsts:
        turns = {0: first}
        bit = dp // 2
        while bit:
            for turn in list(turns):
                turns[turn ^ bit] = lax.ppermute(
                    turns[turn], "dp", [(i, i ^ bit) for i in range(dp)]
                )
            bit //= 2
        pieces.extend(turns[turn] for turn in range(dp))

    keys = own_kv + other_kv
    gain = head_gain[None, :]
    other_branch = attend(lambdas, other_queries, other_gate, gain, keys)
    returned = [
        shifted(other_branch[(step - 1) * rows : step * rows], "tp", tp, tp - step)
        for step in steps
    ]
    own_branch = attend(lambdas, own_queries, own_gate, gain, keys)
    branches = [own_branch, *returned]
    result = tail(branches, out_weight, pieces, out_gate, post_gain[None, :], tp, dp)
    return result[None]


def solution(mesh):
    return jax.shard_map(
        functools.partial(local, mesh.shape["sp"], mesh.shape["tp"], mesh.shape["dp"]),
        mesh=mesh,
        in_specs=(
            P("dp", ("sp", "tp"), None),
            P("dp", ("sp", "tp")),
            P("dp", ("sp", "tp"), None),
            P(("sp", "tp")),
            P(("sp", "tp"), None),
            P(("sp", "tp"), None),
            P(("sp", "tp"), None),
            P(),
            P(),
            P(None, "tp"),
            P(),
            P(),
            P(None, "tp"),
            P("tp"),
            P(),
            P(None, "tp"),
        ),
        out_specs=P("dp", ("sp", "tp"), None),
        check_vma=False,
    )
```
